32 devices in a mesh: ep: 8 (over z, x), tp: 4 (over y, core).
Axes of the slice: x: 2, y: 2, z: 4, core: 2. Of those that a mesh axis runs over, the one named last changes fastest.
Arguments:
- q_in: bfloat16 [4096, 1024], P('ep', 'tp'), may hold values from -6 to 6
- k_in: bfloat16 [4096, 256], P('ep'), may hold values from -6 to 6
- v_in: bfloat16 [4096, 256], P('ep'), may hold values from -6 to 6
- q_gain: float32 [64], replicated, may hold values from 0.1 to 1.9
- k_gain: float32 [64], replicated, may hold values from 0.1 to 1.9
- w_out: bfloat16 [1024, 2048], P('tp'), may hold values from -0.1875 to 0.1875
- post_gain: float32 [2048], replicated, may hold values from 0.1 to 1.9
- moe_in: bfloat16 [1024, 2048], P('ep'), may hold values from -6 to 6
- routes: int32 [1024, 2], P('ep'), may hold values from 0 to 7, all different within a row; in each aligned block of 128 rows (0 to 127, 128 to 255, ...) at most 48 rows name the same one
- route_logits: float32 [1024, 2], P('ep'), may hold values from -6 to 6
- pre_gain: float32 [2048], replicated, may hold values from 0.1 to 1.9
- w_gate: bfloat16 [8, 2048, 4096], P('ep', None, 'tp'), may hold values from -0.125 to 0.125
- w_up: bfloat16 [8, 2048, 4096], P('ep', None, 'tp'), may hold values from -0.125 to 0.125
- w_down: bfloat16 [8, 4096, 2048], P('ep', 'tp'), may hold values from -0.125 to 0.125
Outputs:
- attn_out: bfloat16 [4096, 2048], P(('ep', 'tp'))
- moe_out: bfloat16 [1024, 2048], P('ep', 'tp')
The draws below stay inside these ranges and needn't reach their ends.
Inputs may be any that keep to these rules, and one draw needn't show every extreme that they name: `routes`: each row names 2 different experts. Among the rows of one index of ep no expert is named by more than 48 rows, a bound that some block reaches of them.
All inputs are finite; a program needn't handle non-finite values.
Results may differ from the reference program's by a relative error of at most 0.018.
Values may be sent and summed in bfloat16 or wider, within the bound.
No kernel may reach another device: no remote copies, remote signals or barrier semaphores. Data moves between devices by JAX's collectives and lax.ppermute only.
A program may use at most 64 MiB of HBM per device.

```python
import math
import jax
import jax.numpy as jnp
import numpy as np
from jax import lax

D = 2048
HEADS = 16
KV_HEADS = 4
HEAD = 64
GRID_W = 128
FFE = 4096
TOP = 2
TOKM_DEV = 128
SEQ = 4096
TOKM = 1024
EXPERTS = 8
HEADS_DEV = 4
FF_DEV = 1024
CAP = 48
N_EP = 8
N_TP = 4


def strengthened(drawn, own_key, source, target, shards_of, factor):
    def block_of(axis_at):
        return (jnp.arange(drawn.shape[axis_at]) // (drawn.shape[axis_at] // shards_of)).reshape((-1,) + (1,) * (drawn.ndim - 1 - axis_at))

    one_side = jax.random.permutation(own_key, shards_of)[block_of(target)]
    far = (block_of(target) + shards_of // 2) % shards_of
    return jnp.where((block_of(source) == one_side) | (block_of(source) == far), factor * drawn, drawn)


def block_levels(key, extent, shards, low, largest):
    factor_of, own = 1.0, jax.random.fold_in(key, 6)
    for dim, shards_of in shards:
        heights = jnp.exp(jax.random.uniform(jax.random.fold_in(own, dim), (shards_of,), jnp.float32, low / len(shards), largest / len(shards)))
        factor_of = factor_of * jnp.repeat(heights, extent[dim] // shards_of).reshape([-1 if axis == dim else 1 for axis in range(len(extent))])
    return factor_of


def assign_block(own_key, own, number, rows, number_of, top, bound, slope):
    order = jax.random.permutation(own_key, number_of)
    heavy_load, usual = load_shares(number_of, rows * top, bound, slope, True), load_shares(number_of, rows * top, bound, slope, False)
    places = jnp.arange(number_of)

    def named(lengths, offset_by):
        used = int((lengths > 0).sum())
        fixed = max(1, used // 4)
        shifted = fixed + (places - fixed + offset_by * (used - fixed)) % max(1, number_of - fixed)
        return jnp.zeros((number_of,), jnp.int32).at[order[jnp.where(places < fixed, places, shifted)]].set(jnp.asarray(lengths, jnp.int32))

    lengths = jnp.where(number % 4 == 0, named(heavy_load, number // 4), named(usual, number - number // 4 - 1))
    mixed = jax.random.permutation(jax.random.fold_in(own, 3), number_of)
    source_of, taker = mixed[0:number_of // 2 * 2:2], mixed[1:number_of // 2 * 2:2]
    margin = jnp.minimum(lengths[source_of] - 1, bound - lengths[taker]) // 2
    margin = jnp.where((source_of == order[0]) | (taker == order[0]) | (lengths[taker] == 0), 0, jnp.maximum(margin, 0))
    shifted = jax.random.randint(jax.random.fold_in(own, 4), (number_of // 2,), 0, 1 << 20) % (margin + 1)
    lengths = lengths.at[source_of].add(-shifted).at[taker].add(shifted)
    labels = jnp.searchsorted(jnp.cumsum(lengths), jnp.arange(rows * top), side="right").astype(jnp.int32)
    grid = labels.reshape(top, rows).T
    grid = grid[jax.random.permutation(jax.random.fold_in(own, 1), rows)]
    offset_by = jax.random.randint(jax.random.fold_in(own, 2), (rows, 1), 0, top)
    return jnp.take_along_axis(grid, (jnp.arange(top)[None, :] + offset_by) % top, axis=1)


def load_shares(number_of, total, limit, slope, full):
    weights = [(1 << 20) // math.isqrt(rank ** slope) + 1 for rank in range(1, number_of + 1)]
    largest = limit if full else min(limit, max(-(-total // number_of), total * weights[0] // sum(weights)))
    least = 1 if total - largest >= number_of - 1 else 0
    given, surplus = [largest] + [least] * (number_of - 1), total - largest - least * (number_of - 1)
    while surplus > 0:
        movable = [i for i in range(1, number_of) if given[i] < largest] or [i for i in range(1, number_of) if given[i] < limit]
        pool, budget = sum([weights[i] for i in movable]), surplus
        for i in movable:
            extra = min(limit - given[i], max(1, budget * weights[i] // pool), surplus)
            given[i] = given[i] + extra
            surplus = surplus - extra
    return np.array(given)


def noise(stream_key, extent, deviation, reach, cuts=(), kind=jnp.bfloat16):
    drawn = deviation * jax.random.normal(stream_key, extent, jnp.float32)
    if cuts:
        drawn = drawn * block_levels(stream_key, extent, cuts, -0.22, 0.18)
    return jnp.clip(drawn, -reach, reach).astype(kind)


def heavy_noise(own_key, dims, deviation, most, pieces, heavy, held_as=jnp.bfloat16):
    result = deviation * jax.random.normal(own_key, dims, jnp.float32)
    if pieces:
        result = result * block_levels(own_key, dims, pieces, -0.22, 0.18)
    return jnp.clip(strengthened(result, jax.random.fold_in(own_key, 3), *heavy), -most, most).astype(held_as)


def setup_inputs(seed: int = 0) -> dict:
    arg_keys = jax.random.split(jax.random.key(seed), 15)
    q_in = noise(arg_keys[0], (SEQ, HEADS * HEAD), 1.0, 6.0, ((0, 8), (1, 4)))
    k_in = noise(arg_keys[1], (SEQ, KV_HEADS * HEAD), 1.0, 6.0, ((0, 8),))
    v_in = noise(arg_keys[2], (SEQ, KV_HEADS * HEAD), 1.0, 6.0, ((0, 8),))
    q_gain = jnp.clip(1.0 + 0.18 * jax.random.normal(arg_keys[3], (HEAD,), jnp.float32), 0.1, 1.9)
    k_gain = jnp.clip(1.0 + 0.18 * jax.random.normal(arg_keys[4], (HEAD,), jnp.float32), 0.1, 1.9)
    w_out = noise(arg_keys[5], (HEADS * HEAD, D), (HEADS * HEAD) ** -0.5, 0.1875, ((0, 4),))
    post_gain = jnp.clip(1.0 + 0.18 * jax.random.normal(arg_keys[6], (D,), jnp.float32), 0.1, 1.9)
    moe_in = noise(arg_keys[7], (TOKM, D), 1.0, 6.0, ((0, 8),))
    routes_keys = jax.random.split(jax.random.fold_in(arg_keys[8], 1), TOKM // TOKM_DEV)
    routes_turns = jax.random.permutation(jax.random.fold_in(arg_keys[8], 3), TOKM // TOKM_DEV)
    routes = jax.vmap(lambda own, number: assign_block(jax.random.fold_in(arg_keys[8], 2), own, number, TOKM_DEV, EXPERTS, TOP, CAP, 2))(routes_keys, routes_turns).reshape((TOKM, TOP))
    route_logits = noise(arg_keys[9], (TOKM, TOP), 1.5, 6.0, ((0, 8),), jnp.float32)
    pre_gain = jnp.clip(1.0 + 0.18 * jax.random.normal(arg_keys[10], (D,), jnp.float32), 0.1, 1.9)
    w_gate = noise(arg_keys[11], (EXPERTS, D, FFE), D ** -0.5, 0.125, ((0, 8), (2, 4)))
    w_up = noise(arg_keys[12], (EXPERTS, D, FFE), D ** -0.5, 0.125, ((0, 8), (2, 4)))
    w_down = heavy_noise(arg_keys[13], (EXPERTS, FFE, D), FFE ** -0.5, 0.125, ((0, 8), (1, 4)), (1, 2, 4, 2.0))
    return {"q_in": q_in, "k_in": k_in, "v_in": v_in, "q_gain": q_gain, "k_gain": k_gain, "w_out": w_out, "post_gain": post_gain, "moe_in": moe_in, "routes": routes, "route_logits": route_logits, "pre_gain": pre_gain, "w_gate": w_gate, "w_up": w_up, "w_down": w_down}


EPSILON = 1e-06
ROPE_BASE = 10000.0

def head_norm(values, gain):
    return values * lax.rsqrt(lax.optimization_barrier(jnp.mean(values * values, axis=-1, keepdims=True)) + EPSILON) * gain

def rotate_half(values, angles):
    quarter = angles.shape[-1]
    first_part = values[..., :quarter]
    second_part = values[..., quarter:]
    cosine = jnp.cos(angles)[:, None, :]
    sine_part = jnp.sin(angles)[:, None, :]
    return jnp.concatenate([first_part * cosine - second_part * sine_part, second_part * cosine + first_part * sine_part], axis=-1)

def grid_rotary(values, offset):
    row_count = values.shape[0]
    head_width = values.shape[-1]
    quarter = head_width // 4
    half_width = head_width // 2
    position = offset + jnp.arange(row_count, dtype=jnp.int32)
    grid_row = (position // GRID_W).astype(jnp.float32)
    grid_col = (position % GRID_W).astype(jnp.float32)
    inverse = ROPE_BASE ** (-jnp.arange(quarter, dtype=jnp.float32) / quarter)
    return jnp.concatenate([rotate_half(values[..., :half_width], grid_row[:, None] * inverse[None, :]), rotate_half(values[..., half_width:], grid_col[:, None] * inverse[None, :])], axis=-1)

def slot_table(route_rows, expert_count, capacity):
    token_count, top_count = route_rows.shape
    flat_routes = route_rows.reshape(-1).astype(jnp.int32)
    one_hot = (flat_routes[:, None] == jnp.arange(expert_count, dtype=jnp.int32)[None, :]).astype(jnp.int32)
    ranked = lax.optimization_barrier(jnp.sum((jnp.cumsum(one_hot, axis=0) - 1) * one_hot, axis=1))
    placed = (flat_routes * capacity + ranked).astype(jnp.int32)
    slot_owner = jnp.full((expert_count * capacity,), token_count * top_count, dtype=jnp.int32)
    slot_owner = slot_owner.at[placed].set(jnp.arange(token_count * top_count, dtype=jnp.int32))
    return (slot_owner, placed)

def mixer_half(q_in, k_in, v_in, q_gain, k_gain, w_out, post_gain):
    queries = head_norm(q_in.astype(jnp.float32).reshape(SEQ, HEADS, HEAD), q_gain.astype(jnp.float32))
    queries = grid_rotary(queries, 0).astype(jnp.bfloat16)
    keys = head_norm(k_in.astype(jnp.float32).reshape(SEQ, KV_HEADS, HEAD), k_gain.astype(jnp.float32))
    keys = grid_rotary(keys, 0).astype(jnp.bfloat16)
    repeat = HEADS // KV_HEADS
    key_float = keys.astype(jnp.float32)
    value_float = v_in.astype(jnp.float32).reshape(SEQ, KV_HEADS, HEAD)
    blocked = queries.reshape(SEQ // 128, 128, KV_HEADS, repeat, HEAD)

    def attend(query_block):
        scores = jnp.einsum('qgrd,kgd->grqk', query_block.astype(jnp.float32), key_float) * HEAD ** (-0.5)
        weights = jnp.exp(scores)
        denominator = lax.optimization_barrier(jnp.sum(weights, axis=-1))
        rounded = lax.optimization_barrier(weights.astype(jnp.bfloat16)).astype(jnp.float32)
        summed = jnp.einsum('grqk,kgd->qgrd', rounded, value_float)
        return (summed / jnp.transpose(denominator, (2, 0, 1))[..., None]).astype(jnp.bfloat16)
    head_out = lax.map(attend, blocked).reshape(SEQ, HEADS * HEAD)
    grouped_out = head_out.reshape(SEQ, N_TP, HEADS_DEV * HEAD)
    grouped_w = w_out.reshape(N_TP, HEADS_DEV * HEAD, D)

    def add_group(running, index):
        term = jnp.dot(grouped_out[:, index], grouped_w[index], preferred_element_type=jnp.float32)
        term = lax.optimization_barrier(term.astype(jnp.bfloat16))
        return (running + term.astype(jnp.float32), None)
    mixed, unused = lax.scan(add_group, jnp.zeros((SEQ, D), jnp.float32), jnp.arange(N_TP, dtype=jnp.int32))
    return head_norm(mixed, post_gain.astype(jnp.float32)).astype(jnp.bfloat16)

def experts_half(moe_in, routes, route_logits, pre_gain, w_gate, w_up, w_down):
    normed = head_norm(moe_in.astype(jnp.float32), pre_gain.astype(jnp.float32)).astype(jnp.bfloat16)
    copy_count = TOKM * TOP
    local_copies = TOKM_DEV * TOP
    padded = jnp.concatenate([normed, jnp.zeros((1, D), normed.dtype)], axis=0)
    blocks = routes.reshape(N_EP, TOKM_DEV, TOP)
    owners, unused = jax.vmap(lambda block_routes: slot_table(block_routes, EXPERTS, CAP))(blocks)
    shift_by = (jnp.arange(N_EP, dtype=jnp.int32) * local_copies)[:, None]
    global_owner = jnp.where(owners < local_copies, owners + shift_by, copy_count).astype(jnp.int32)
    per_expert = global_owner.reshape(N_EP, EXPERTS, CAP).transpose(1, 0, 2).reshape(EXPERTS, N_EP * CAP)

    def one_expert(results, inputs):
        owner_ids, gate_w, up_w, down_w = inputs
        gathered = padded[owner_ids // TOP]
        gate_pre = jnp.dot(gathered, gate_w, preferred_element_type=jnp.float32)
        up_pre = jnp.dot(gathered, up_w, preferred_element_type=jnp.float32)
        hidden = (jax.nn.silu(gate_pre) * up_pre).astype(jnp.bfloat16)
        hidden_groups = hidden.reshape(N_EP * CAP, N_TP, FF_DEV)
        down_groups = down_w.reshape(N_TP, FF_DEV, D)

        def add_group(running, index):
            term = jnp.dot(hidden_groups[:, index], down_groups[index], preferred_element_type=jnp.float32)
            term = lax.optimization_barrier(term.astype(jnp.bfloat16))
            return (running + term.astype(jnp.float32), None)
        combined, unused_out = lax.scan(add_group, jnp.zeros((N_EP * CAP, D), jnp.float32), jnp.arange(N_TP, dtype=jnp.int32))
        return (results.at[owner_ids].set(combined.astype(results.dtype)), None)
    results, unused_all = lax.scan(one_expert, jnp.zeros((copy_count + 1, D), jnp.bfloat16), (per_expert, w_gate, w_up, w_down))
    copies = results[:copy_count].reshape(TOKM, TOP, D).astype(jnp.float32)
    route_weight = jax.nn.softmax(route_logits.astype(jnp.float32), axis=-1)
    return lax.optimization_barrier(jnp.sum(route_weight[..., None] * copies, axis=1)).astype(jnp.bfloat16)

def reference(q_in, k_in, v_in, q_gain, k_gain, w_out, post_gain, moe_in, routes, route_logits, pre_gain, w_gate, w_up, w_down):
    attn_out = mixer_half(q_in, k_in, v_in, q_gain, k_gain, w_out, post_gain)
    moe_out = experts_half(moe_in, routes, route_logits, pre_gain, w_gate, w_up, w_down)
    return (attn_out, moe_out)
```

```python
import functools
import jax
import jax.numpy as jnp
from jax import lax
from jax.experimental import pallas as pl
from jax.experimental.pallas import tpu as pltpu
from jax.sharding import PartitionSpec as P

GRID_W = 128
EPSILON = 1e-06
ROPE_BASE = 10000.0
LOG2E = 1.4426950408889634
BF = jnp.bfloat16
F32 = jnp.float32


def head_norm(values, gain):
    return values * lax.rsqrt(jnp.mean(values * values, axis=-1, keepdims=True) + EPSILON) * gain


def swap(value, axis, step):
    count = lax.axis_size(axis)
    return lax.ppermute(value, axis, [(i, i ^ step) for i in range(count)])


def grid_rotary(values, offset):
    rows, heads, size = values.shape
    quarter = size // 4
    position = offset + jnp.arange(rows, dtype=jnp.int32)
    place = jnp.stack([position // GRID_W, position % GRID_W], axis=1).astype(F32)
    inverse = ROPE_BASE ** (-jnp.arange(quarter, dtype=F32) / quarter)
    angles = place[:, :, None] * inverse[None, None, :]
    cosine = jnp.cos(angles)
    sine = jnp.sin(angles)
    cos_full = jnp.concatenate([cosine, cosine], axis=2).reshape(rows, 1, size)
    sin_full = jnp.concatenate([-sine, sine], axis=2).reshape(rows, 1, size)
    parts = [values[..., i * quarter:(i + 1) * quarter] for i in (1, 0, 3, 2)]
    return values * cos_full + jnp.concatenate(parts, axis=-1) * sin_full


def attend_body(blk_ref, q_ref, w_ref, *refs, pieces, size):
    kv_refs, out_ref = refs[:pieces], refs[pieces]
    heads, rows, width = q_ref.shape
    queries = q_ref[...].reshape(heads * rows, width)
    acc = jnp.zeros((heads * rows, width), F32)
    for kv_ref in kv_refs:
        kv = kv_ref[...]
        scores = lax.dot_general(queries, kv, (((1,), (1,)), ((), ())), preferred_element_type=F32)
        weights = jnp.exp2(scores).astype(BF)
        lane = lax.broadcasted_iota(jnp.int32, kv.shape, 1)
        ones_and_values = jnp.where(lane < size, jnp.ones_like(kv), kv)
        acc = acc + jnp.dot(weights, ones_and_values, preferred_element_type=F32)
    head_out = (acc[:, size:] / acc[:, :size]).astype(BF)
    merged = jnp.concatenate([head_out[h * rows:(h + 1) * rows] for h in range(heads)], axis=1)
    out_ref[0] = jnp.dot(merged, w_ref[...], preferred_element_type=F32).astype(BF)


def attend(queries, kv_pieces, w_out, blocks, size):
    heads, row_count, width = queries.shape
    rows = row_count // lax.axis_size("tp")
    count = blocks.shape[0]
    keys = kv_pieces[0].shape[0]
    model = w_out.shape[1]
    total = heads * rows * count * keys * len(kv_pieces)
    return pl.pallas_call(
        functools.partial(attend_body, pieces=len(kv_pieces), size=size),
        grid_spec=pltpu.PrefetchScalarGridSpec(
            num_scalar_prefetch=1,
            grid=(count,),
            in_specs=[
                pl.BlockSpec((heads, rows, width), lambda i, blk: (0, blk[i], 0)),
                pl.BlockSpec(w_out.shape, lambda i, blk: (0, 0)),
            ]
            + [pl.BlockSpec((keys, width), lambda i, blk: (0, 0)) for _ in kv_pieces],
            out_specs=pl.BlockSpec((1, rows, model), lambda i, blk: (i, 0, 0)),
        ),
        out_shape=jax.ShapeDtypeStruct((count, rows, model), BF),
        cost_estimate=pl.CostEstimate(
            flops=total * 2 * width * 2, transcendentals=total,
            bytes_accessed=2 * (keys * len(kv_pieces) * width + w_out.size),
        ),
        name="attend",
    )(blocks, queries, w_out, *kv_pieces)


def sum_norm_body(gain_ref, *refs):
    out_ref = refs[-1]
    total = refs[0][...].astype(F32)
    for ref in refs[1:-1]:
        total = total + ref[...].astype(F32)
    out_ref[...] = head_norm(total, gain_ref[...]).astype(BF)


def pieces_of(paired):
    count = lax.axis_size("ep")
    return [paired] + [swap(paired, "ep", s) for s in range(1, count)]


def attention_inputs(q_in, k_in, v_in, q_gain, k_gain):
    size = q_gain.shape[0]
    row_count = q_in.shape[0]
    heads = q_in.shape[1] // size
    kv_count = k_in.shape[1] // size
    repeat = heads * lax.axis_size("tp") // kv_count
    offset = lax.axis_index("ep") * row_count
    kv_index = lax.axis_index("tp") * heads // repeat
    own_keys = lax.dynamic_slice_in_dim(k_in, kv_index * size, size, 1)
    own_values = lax.dynamic_slice_in_dim(v_in, kv_index * size, size, 1)
    own_keys = head_norm(own_keys.astype(F32)[:, None, :], k_gain)
    own_keys = grid_rotary(own_keys, offset)[:, 0, :].astype(BF)
    paired = jnp.concatenate([own_keys, own_values], axis=1)
    queries = head_norm(q_in.astype(F32).reshape(row_count, heads, size), q_gain)
    queries = (grid_rotary(queries, offset) * (LOG2E * size ** (-0.5))).astype(BF)
    queries = jnp.transpose(queries, (1, 0, 2))
    queries = jnp.pad(queries, ((0, 0), (0, 0), (0, size)))
    return queries, paired


def attention_tail(queries, kv_pieces, w_out, post_gain, size):
    tp = lax.axis_size("tp")
    own = lax.axis_index("tp").astype(jnp.int32)
    odd = attend(queries, kv_pieces, w_out, own ^ jnp.arange(1, tp, 2, dtype=jnp.int32), size)
    got = swap(odd, "tp", 1)
    far = attend(queries, kv_pieces, w_out, own ^ jnp.arange(2, tp, 2, dtype=jnp.int32), size)
    terms = []
    for j in range(1, tp // 2):
        pair = (far[j - 1].astype(F32) + got[j].astype(F32)).astype(BF)
        terms.append(swap(pair, "tp", 2 * j))
    near = attend(queries, kv_pieces, w_out, own[None], size)
    terms = [near[0], got[0]] + terms
    return pl.pallas_call(
        sum_norm_body,
        out_shape=jax.ShapeDtypeStruct(terms[0].shape, BF),
        name="sum_norm",
    )(post_gain[None, :], *terms)


def dispatch_body(core_ref, x_ref, gain_ref, sel_ref, out_ref, normed):
    width = out_ref.shape[1]
    normed[...] = head_norm(x_ref[...].astype(F32), gain_ref[...]).astype(BF)
    start = pl.multiple_of(core_ref[0] * width, 128)
    half = normed[:, pl.ds(start, width)]
    out_ref[...] = jnp.dot(sel_ref[...], half, preferred_element_type=F32).astype(BF)


def expert_body(own_ref, a_ref, b_ref, g_ref, u_ref, d_ref, send_ref, keep_ref, acc):
    step = pl.program_id(0)
    own = own_ref[0]
    half = a_ref.shape[1]
    first = pl.multiple_of((own % 2) * half, 128)
    second = pl.multiple_of((1 - own % 2) * half, 128)

    def project(w_ref):
        left = jnp.dot(a_ref[...], w_ref[0, pl.ds(first, half), :], preferred_element_type=F32)
        return left + jnp.dot(b_ref[...], w_ref[0, pl.ds(second, half), :], preferred_element_type=F32)

    gate = project(g_ref)
    up = project(u_ref)
    hidden = (gate / (1.0 + jnp.exp(-gate)) * up).astype(BF)
    down = jnp.dot(hidden, d_ref[0], preferred_element_type=F32)

    @pl.when(step == 0)
    def _():
        acc[...] = down

    @pl.when(step > 0)
    def _():
        acc[...] = acc[...] + down

    @pl.when(step == pl.num_programs(0) - 1)
    def _():
        width = keep_ref.shape[2]
        for j in range(keep_ref.shape[0]):
            at = pl.multiple_of((own ^ (2 * j)) * width, 128)
            keep_ref[j] = acc[:, pl.ds(at, width)].astype(BF)
            at = pl.multiple_of((own ^ (2 * j + 1)) * width, 128)
            send_ref[j] = acc[:, pl.ds(at, width)].astype(BF)


def combine_body(ret_ref, sel_ref, weight_ref, out_ref):
    total = jnp.zeros(out_ref.shape, F32)
    for k in range(sel_ref.shape[0]):
        rows = jnp.dot(sel_ref[k], ret_ref[...], preferred_element_type=F32)
        total = total + weight_ref[:, k:k + 1] * rows
    out_ref[...] = total.astype(BF)


def route_tables(routes, capacity):
    token_count, top = routes.shape
    experts = lax.axis_size("ep")
    named = routes[:, :, None] == jnp.arange(experts, dtype=jnp.int32)
    chosen = jnp.any(named, axis=1)
    before = jnp.tril(jnp.ones((token_count, token_count), BF), -1)
    rank = jnp.dot(before, chosen.astype(BF), preferred_element_type=F32).astype(jnp.int32)
    slot = jnp.arange(experts * capacity, dtype=jnp.int32)
    place = jnp.where(chosen, rank + jnp.arange(experts, dtype=jnp.int32) * capacity, -1)
    fill = jnp.repeat(place.T, capacity, axis=0) == slot[:, None]
    placed = jnp.sum(jnp.where(named, place[:, None, :], 0), axis=2)
    pick = placed.T[:, :, None] == slot
    return fill.astype(BF), pick.astype(BF)


def experts_send(moe_in, routes, pre_gain):
    token_count, top = routes.shape
    model = moe_in.shape[1]
    experts = lax.axis_size("ep")
    capacity = max(2, 3 * top * token_count // (2 * experts))
    own = lax.axis_index("tp").astype(jnp.int32)
    fill, pick = route_tables(routes, capacity)
    half = model // 2
    vmem = pl.BlockSpec(memory_space=pltpu.VMEM)
    outgoing = pl.pallas_call(
        dispatch_body,
        in_specs=[pl.BlockSpec(memory_space=pltpu.SMEM), vmem, vmem, vmem],
        out_specs=vmem,
        out_shape=jax.ShapeDtypeStruct((experts * capacity, half), BF),
        scratch_shapes=[pltpu.VMEM((token_count, model), BF)],
        name="dispatch",
    )((own % 2)[None], moe_in, pre_gain[None, :], fill)
    return outgoing.reshape(experts, capacity, half), pick


def experts_compute(first, second, w_gate, w_up, w_down):
    slots, half = first.shape
    model = 2 * half
    hidden = w_gate.shape[2]
    tp = lax.axis_size("tp")
    own = lax.axis_index("tp").astype(jnp.int32)
    chunk = min(256, hidden)
    shape = jax.ShapeDtypeStruct((tp // 2, slots, model // tp), BF)
    whole = pl.BlockSpec((slots, half), lambda i, o: (0, 0))
    result = pl.BlockSpec(shape.shape, lambda i, o: (0, 0, 0))
    return pl.pallas_call(
        expert_body,
        grid_spec=pltpu.PrefetchScalarGridSpec(
            num_scalar_prefetch=1,
            grid=(hidden // chunk,),
            in_specs=[
                whole,
                whole,
                pl.BlockSpec((1, model, chunk), lambda i, o: (0, 0, i)),
                pl.BlockSpec((1, model, chunk), lambda i, o: (0, 0, i)),
                pl.BlockSpec((1, chunk, model), lambda i, o: (0, i, 0)),
            ],
            out_specs=[result, result],
            scratch_shapes=[pltpu.VMEM((slots, model), F32)],
        ),
        out_shape=[shape, shape],
        cost_estimate=pl.CostEstimate(
            flops=6 * slots * model * hidden, transcendentals=slots * hidden,
            bytes_accessed=6 * model * hidden,
        ),
        name="experts",
    )(own[None], first, second, w_gate, w_up, w_down)


def per_device(
    q_in, k_in, v_in, q_gain, k_gain, w_out, post_gain,
    moe_in, routes, route_logits, pre_gain, w_gate, w_up, w_down,
):
    tp = lax.axis_size("tp")
    size = q_gain.shape[0]
    queries, paired = attention_inputs(q_in, k_in, v_in, q_gain, k_gain)
    outgoing, pick = experts_send(moe_in, routes, pre_gain)
    route_weight = jax.nn.softmax(route_logits, axis=-1)
    kv_pieces = pieces_of(paired)
    arrived = lax.all_to_all(outgoing, "ep", split_axis=0, concat_axis=0, tiled=True)
    arrived = arrived.reshape(-1, arrived.shape[2])
    partner = swap(arrived, "tp", 1)
    attn_out = attention_tail(queries, kv_pieces, w_out, post_gain, size)
    send, keep = experts_compute(arrived, partner, w_gate, w_up, w_down)
    got = swap(send, "tp", 1)
    total = keep[0].astype(F32) + got[0].astype(F32)
    for j in range(1, tp // 2):
        pair = (keep[j].astype(F32) + got[j].astype(F32)).astype(BF)
        total = total + swap(pair, "tp", 2 * j).astype(F32)
    experts, capacity, _ = outgoing.shape
    summed = total.astype(BF).reshape(experts, capacity, -1)
    returned = lax.all_to_all(summed, "ep", split_axis=0, concat_axis=0, tiled=True)
    returned = returned.reshape(experts * capacity, -1)
    moe_out = pl.pallas_call(
        combine_body,
        out_shape=jax.ShapeDtypeStruct((routes.shape[0], returned.shape[1]), BF),
        name="combine",
    )(returned, pick, route_weight)
    return (attn_out, moe_out)


def solution(mesh):
    return jax.shard_map(
        per_device,
        mesh=mesh,
        in_specs=(
            P("ep", "tp"), P("ep", None), P("ep", None), P(), P(), P("tp", None), P(),
            P("ep", None), P("ep", None), P("ep", None), P(),
            P("ep", None, "tp"), P("ep", None, "tp"), P("ep", "tp", None),
        ),
        out_specs=(P(("ep", "tp"), None), P("ep", "tp")),
        check_vma=False,
    )
```

```python
import functools
import jax
import jax.numpy as jnp
from jax import lax
from jax.experimental import pallas as pl
from jax.experimental.pallas import tpu as pltpu
from jax.sharding import PartitionSpec as P

GRID_W = 128
EPSILON = 1e-06
ROPE_BASE = 10000.0
LOG2E = 1.4426950408889634
BF = jnp.bfloat16
F32 = jnp.float32


def head_norm(values, gain):
    return values * lax.rsqrt(jnp.mean(values * values, axis=-1, keepdims=True) + EPSILON) * gain


def swap(value, axis, step):
    count = lax.axis_size(axis)
    return lax.ppermute(value, axis, [(i, i ^ step) for i in range(count)])


def grid_rotary(values, offset):
    rows, _, size = values.shape
    quarter = size // 4
    position = offset + jnp.arange(rows, dtype=jnp.int32)
    place = jnp.stack([position // GRID_W, position % GRID_W], axis=1).astype(F32)
    inverse = ROPE_BASE ** (-jnp.arange(quarter, dtype=F32) / quarter)
    angles = place[:, :, None] * inverse[None, None, :]
    cosine = jnp.cos(angles)
    sine = jnp.sin(angles)
    cos_full = jnp.concatenate([cosine, cosine], axis=2).reshape(rows, 1, size)
    sin_full = jnp.concatenate([-sine, sine], axis=2).reshape(rows, 1, size)
    parts = [values[..., i * quarter:(i + 1) * quarter] for i in (1, 0, 3, 2)]
    return values * cos_full + jnp.concatenate(parts, axis=-1) * sin_full


def attend_body(blk_ref, q_ref, w_ref, *refs, pieces, size):
    kv_refs, out_ref = refs[:pieces], refs[pieces]
    heads, rows, width = q_ref.shape
    queries = q_ref[...].reshape(heads * rows, width)
    acc = jnp.zeros((heads * rows, width), F32)
    for kv_ref in kv_refs:
        kv = kv_ref[...]
        scores = lax.dot_general(queries, kv, (((1,), (1,)), ((), ())), preferred_element_type=F32)
        weights = jnp.exp2(scores).astype(BF)
        lane = lax.broadcasted_iota(jnp.int32, kv.shape, 1)
        ones_and_values = jnp.where(lane < size, jnp.ones_like(kv), kv)
        acc = acc + jnp.dot(weights, ones_and_values, preferred_element_type=F32)
    head_out = (acc[:, size:] / acc[:, :size]).astype(BF)
    merged = jnp.concatenate([head_out[h * rows:(h + 1) * rows] for h in range(heads)], axis=1)
    out_ref[0] = jnp.dot(merged, w_ref[...], preferred_element_type=F32).astype(BF)


def attend(queries, kv_pieces, w_out, blocks, size):
    heads, row_count, width = queries.shape
    rows = row_count // lax.axis_size("tp")
    count = blocks.shape[0]
    keys = kv_pieces[0].shape[0]
    model = w_out.shape[1]
    total = heads * rows * count * keys * len(kv_pieces)
    return pl.pallas_call(
        functools.partial(attend_body, pieces=len(kv_pieces), size=size),
        grid_spec=pltpu.PrefetchScalarGridSpec(
            num_scalar_prefetch=1,
            grid=(count,),
            in_specs=[
                pl.BlockSpec((heads, rows, width), lambda i, blk: (0, blk[i], 0)),
                pl.BlockSpec(w_out.shape, lambda i, blk: (0, 0)),
            ]
            + [pl.BlockSpec((keys, width), lambda i, blk: (0, 0)) for _ in kv_pieces],
            out_specs=pl.BlockSpec((1, rows, model), lambda i, blk: (i, 0, 0)),
        ),
        out_shape=jax.ShapeDtypeStruct((count, rows, model), BF),
        cost_estimate=pl.CostEstimate(
            flops=total * 2 * width * 2, transcendentals=total,
            bytes_accessed=2 * (keys * len(kv_pieces) * width + w_out.size),
        ),
        name="attend",
    )(blocks, queries, w_out, *kv_pieces)


def pad_body(in_ref, out_ref):
    value = in_ref[...]
    out_ref[...] = jnp.concatenate([value, jnp.zeros_like(value)], axis=2)


def sum_norm_body(gain_ref, *refs):
    out_ref = refs[-1]
    total = refs[0][...].astype(F32)
    for ref in refs[1:-1]:
        total = total + ref[...].astype(F32)
    out_ref[...] = head_norm(total, gain_ref[...]).astype(BF)


def pieces_of(paired):
    count = lax.axis_size("ep")
    return [paired] + [swap(paired, "ep", s) for s in range(1, count)]


def attention_inputs(q_in, k_in, v_in, q_gain, k_gain):
    size = q_gain.shape[0]
    row_count = q_in.shape[0]
    heads = q_in.shape[1] // size
    kv_count = k_in.shape[1] // size
    repeat = heads * lax.axis_size("tp") // kv_count
    offset = lax.axis_index("ep") * row_count
    kv_index = lax.axis_index("tp") * heads // repeat
    own_keys = lax.dynamic_slice_in_dim(k_in, kv_index * size, size, 1)
    own_values = lax.dynamic_slice_in_dim(v_in, kv_index * size, size, 1)
    own_keys = head_norm(own_keys.astype(F32)[:, None, :], k_gain)
    own_keys = grid_rotary(own_keys, offset)[:, 0, :].astype(BF)
    paired = jnp.concatenate([own_keys, own_values], axis=1)
    queries = head_norm(q_in.astype(F32).reshape(row_count, heads, size), q_gain)
    queries = (grid_rotary(queries, offset) * (LOG2E * size ** (-0.5))).astype(BF)
    queries = jnp.transpose(queries, (1, 0, 2))
    queries = pl.pallas_call(
        pad_body,
        out_shape=jax.ShapeDtypeStruct((heads, row_count, 2 * size), BF),
        name="q_pad",
    )(queries)
    return queries, paired


def after(value, *others):
    return lax.optimization_barrier((value,) + others)[0]


def joined(post_gain, terms):
    return pl.pallas_call(
        sum_norm_body,
        out_shape=jax.ShapeDtypeStruct(terms[0].shape, BF),
        name="sum_norm",
    )(post_gain[None, :], *terms)


def pair_sum(kept, got):
    return (kept.astype(F32) + got.astype(F32)).astype(BF)


def dispatch_body(core_ref, x_ref, gain_ref, sel_ref, out_ref, normed):
    width = out_ref.shape[1]
    normed[...] = head_norm(x_ref[...].astype(F32), gain_ref[...]).astype(BF)
    start = pl.multiple_of(core_ref[0] * width, 128)
    half = normed[:, pl.ds(start, width)]
    out_ref[...] = jnp.dot(sel_ref[...], half, preferred_element_type=F32).astype(BF)


def expert_body(own_ref, a_ref, b_ref, g_ref, u_ref, d_ref, send_ref, keep_ref, acc):
    step = pl.program_id(0)
    own = own_ref[0]
    half = a_ref.shape[1]
    first = pl.multiple_of((own % 2) * half, 128)
    second = pl.multiple_of((1 - own % 2) * half, 128)

    def project(w_ref):
        left = jnp.dot(a_ref[...], w_ref[0, pl.ds(first, half), :], preferred_element_type=F32)
        return left + jnp.dot(b_ref[...], w_ref[0, pl.ds(second, half), :], preferred_element_type=F32)

    gate = project(g_ref)
    up = project(u_ref)
    hidden = (gate / (1.0 + jnp.exp(-gate)) * up).astype(BF)
    down = jnp.dot(hidden, d_ref[0], preferred_element_type=F32)

    @pl.when(step == 0)
    def _():
        acc[...] = down

    @pl.when(step > 0)
    def _():
        acc[...] = acc[...] + down

    @pl.when(step == pl.num_programs(0) - 1)
    def _():
        width = keep_ref.shape[2]
        for j in range(keep_ref.shape[0]):
            at = pl.multiple_of((own ^ (2 * j)) * width, 128)
            keep_ref[j] = acc[:, pl.ds(at, width)].astype(BF)
            at = pl.multiple_of((own ^ (2 * j + 1)) * width, 128)
            send_ref[j] = acc[:, pl.ds(at, width)].astype(BF)


def combine_body(ret_ref, sel_ref, weight_ref, out_ref):
    total = jnp.zeros(out_ref.shape, F32)
    for k in range(sel_ref.shape[0]):
        rows = jnp.dot(sel_ref[k], ret_ref[...], preferred_element_type=F32)
        total = total + weight_ref[:, k:k + 1] * rows
    out_ref[...] = total.astype(BF)


def route_tables(routes, capacity):
    token_count, _ = routes.shape
    experts = lax.axis_size("ep")
    named = routes[:, :, None] == jnp.arange(experts, dtype=jnp.int32)
    chosen = jnp.any(named, axis=1)
    before = jnp.tril(jnp.ones((token_count, token_count), BF), -1)
    rank = jnp.dot(before, chosen.astype(BF), preferred_element_type=F32).astype(jnp.int32)
    slot = jnp.arange(experts * capacity, dtype=jnp.int32)
    place = jnp.where(chosen, rank + jnp.arange(experts, dtype=jnp.int32) * capacity, -1)
    fill = jnp.repeat(place.T, capacity, axis=0) == slot[:, None]
    placed = jnp.sum(jnp.where(named, place[:, None, :], 0), axis=2)
    pick = placed.T[:, :, None] == slot
    return fill.astype(BF), pick.astype(BF)


def experts_send(moe_in, routes, pre_gain):
    token_count, top = routes.shape
    model = moe_in.shape[1]
    experts = lax.axis_size("ep")
    capacity = max(2, 3 * top * token_count // (2 * experts))
    own = lax.axis_index("tp").astype(jnp.int32)
    fill, pick = route_tables(routes, capacity)
    half = model // 2
    vmem = pl.BlockSpec(memory_space=pltpu.VMEM)
    outgoing = pl.pallas_call(
        dispatch_body,
        in_specs=[pl.BlockSpec(memory_space=pltpu.SMEM), vmem, vmem, vmem],
        out_specs=vmem,
        out_shape=jax.ShapeDtypeStruct((experts * capacity, half), BF),
        scratch_shapes=[pltpu.VMEM((token_count, model), BF)],
        name="dispatch",
    )((own % 2)[None], moe_in, pre_gain[None, :], fill)
    return outgoing.reshape(experts, capacity, half), pick


def experts_compute(first, second, w_gate, w_up, w_down):
    slots, half = first.shape
    model = 2 * half
    hidden = w_gate.shape[2]
    tp = lax.axis_size("tp")
    own = lax.axis_index("tp").astype(jnp.int32)
    chunk = min(512, hidden)
    shape = jax.ShapeDtypeStruct((tp // 2, slots, model // tp), BF)
    whole = pl.BlockSpec((slots, half), lambda i, o: (0, 0))
    result = pl.BlockSpec(shape.shape, lambda i, o: (0, 0, 0))
    return pl.pallas_call(
        expert_body,
        grid_spec=pltpu.PrefetchScalarGridSpec(
            num_scalar_prefetch=1,
            grid=(hidden // chunk,),
            in_specs=[
                whole,
                whole,
                pl.BlockSpec((1, model, chunk), lambda i, o: (0, 0, i)),
                pl.BlockSpec((1, model, chunk), lambda i, o: (0, 0, i)),
                pl.BlockSpec((1, chunk, model), lambda i, o: (0, i, 0)),
            ],
            out_specs=[result, result],
            scratch_shapes=[pltpu.VMEM((slots, model), F32)],
        ),
        out_shape=[shape, shape],
        cost_estimate=pl.CostEstimate(
            flops=6 * slots * model * hidden, transcendentals=slots * hidden,
            bytes_accessed=6 * model * hidden,
        ),
        name="experts",
    )(own[None], first, second, w_gate, w_up, w_down)


def whole_step(
    q_in, k_in, v_in, q_gain, k_gain, w_out, post_gain,
    moe_in, routes, route_logits, pre_gain, w_gate, w_up, w_down,
):
    tp = lax.axis_size("tp")
    size = q_gain.shape[0]
    queries, paired = attention_inputs(q_in, k_in, v_in, q_gain, k_gain)
    outgoing, pick = experts_send(moe_in, routes, pre_gain)
    route_weight = jax.nn.softmax(route_logits, axis=-1)
    kv_pieces = pieces_of(paired)
    arrived = lax.all_to_all(outgoing, "ep", split_axis=0, concat_axis=0, tiled=True)
    arrived = arrived.reshape(-1, arrived.shape[2])
    arrived, queries, pick, route_weight = lax.optimization_barrier(
        (arrived, queries, pick, route_weight)
    )
    partner = swap(arrived, "tp", 1)
    send, keep = experts_compute(arrived, partner, w_gate, w_up, w_down)
    got = swap(send, "tp", 1)

    own = lax.axis_index("tp").astype(jnp.int32)

    def part(first, last, *others):
        blocks = own ^ jnp.arange(first, last, 2, dtype=jnp.int32)
        return attend(queries, kv_pieces, w_out, after(blocks, *others), size)

    odd_far = part(3, tp, keep)
    got_far = swap(odd_far, "tp", 1)
    got = after(got, odd_far)
    pairs = [pair_sum(keep[j], got[j]) for j in range(1, tp // 2)]
    total = [keep[0], got[0]] + [swap(p, "tp", 2 * (j + 1)) for j, p in enumerate(pairs)]
    far = part(2, tp, *pairs)
    pairs = [pair_sum(far[j], got_far[j]) for j in range(tp // 2 - 1)]
    terms = [swap(p, "tp", 2 * (j + 1)) for j, p in enumerate(pairs)]
    odd_near = part(1, 2, *pairs)
    got_near = swap(odd_near, "tp", 1)
    total = lax.optimization_barrier(tuple(total) + (odd_near,))[:-1]
    experts, capacity, _ = outgoing.shape
    summed = sum(value.astype(F32) for value in total).astype(BF)
    near = part(0, 1, summed)
    summed = summed.reshape(experts, capacity, -1)
    attn_out = joined(post_gain, [near[0], got_near[0]] + terms)
    returned = lax.all_to_all(summed, "ep", split_axis=0, concat_axis=0, tiled=True)
    returned = returned.reshape(experts * capacity, -1)
    moe_out = pl.pallas_call(
        combine_body,
        out_shape=jax.ShapeDtypeStruct((routes.shape[0], returned.shape[1]), BF),
        name="combine",
    )(returned, pick, route_weight)
    return (attn_out, moe_out)


def solution(mesh):
    return jax.shard_map(
        whole_step,
        mesh=mesh,
        in_specs=(
            P("ep", "tp"), P("ep", None), P("ep", None), P(), P(), P("tp", None), P(),
            P("ep", None), P("ep", None), P("ep", None), P(),
            P("ep", None, "tp"), P("ep", None, "tp"), P("ep", "tp", None),
        ),
        out_specs=(P(("ep", "tp"), None), P("ep", "tp")),
        check_vma=False,
    )
```
